32 devices in a mesh: grp: 2 (over x), tp: 4 (over y, core), dp: 4 (over z).
Axes of the slice: x: 2, y: 2, z: 4, core: 2. Of those that a mesh axis runs over, the one named last changes fastest.
Arguments:
- tokens: bfloat16 [64, 4096], P(('grp', 'tp'), 'dp'), parts along dimension 0, may hold values from -45 to 45
- w_in: bfloat16 [2, 2, 4096, 8192], P(None, None, 'dp', 'tp'), may hold values from -0.09375 to 0.09375
- w_vec: bfloat16 [2, 2, 4096, 2048], P(None, None, 'dp', 'tp'), may hold values from -0.09375 to 0.09375
- w_step: bfloat16 [2, 4096, 128], P(None, 'dp'), may hold values from -0.09375 to 0.09375
- conv_weight: bfloat16 [2, 4, 8192], P(None, None, 'tp'), may hold values from -3 to 3
- conv_vec: bfloat16 [2, 2, 4, 2048], P(None, None, None, 'tp'), may hold values from -3 to 3
- conv_state: bfloat16 [2, 64, 3, 8192], P(None, ('grp', 'dp'), None, 'tp'), parts along dimension 1, may hold values from -6 to 6
- vec_state: bfloat16 [2, 2, 64, 3, 2048], P(None, None, ('grp', 'dp'), None, 'tp'), parts along dimension 2, may hold values from -6 to 6
- ssm_state: float32 [2, 64, 128, 64, 128], P(None, ('grp', 'dp'), 'tp'), parts along dimension 1, may hold values from -4 to 4
- step_bias: float32 [2, 128], P(None, 'tp'), may hold values from -1.5 to 1
- decay_log: float32 [2, 128], P(None, 'tp'), may hold values from -4 to 1
- skip_gain: float32 [2, 128], P(None, 'tp'), may hold values from 0.5 to 3
- mix_gain: bfloat16 [2, 4096], P(None, 'dp'), may hold values from 0.099609375 to 1.8984375
- out_gain: bfloat16 [2, 8192], P(None, 'tp'), may hold values from 0.099609375 to 1.8984375
- w_out: bfloat16 [2, 8192, 4096], P(None, 'tp', 'dp'), may hold values from -0.0625 to 0.0625
Outputs:
- new_tokens: bfloat16 [64, 4096], P(('grp', 'tp'), 'dp'), parts along dimension 0
- new_conv: bfloat16 [2, 64, 3, 8192], P(None, ('grp', 'dp'), None, 'tp'), parts along dimension 1
- new_vec: bfloat16 [2, 2, 64, 3, 2048], P(None, None, ('grp', 'dp'), None, 'tp'), parts along dimension 2
- new_ssm: float32 [2, 64, 128, 64, 128], P(None, ('grp', 'dp'), 'tp'), parts along dimension 1
The draws below stay inside these ranges and needn't reach their ends.
There are 2 independent parts, one for each index of `grp`. The reference program is written for one: setup_inputs(seed, part) draws one part's arguments, and reference() takes and returns one part's arrays. A program takes and returns all parts, laid end to end along the dimension named above; an argument that names none is the same for every part. Nothing has to cross between parts.
All inputs are finite; a program needn't handle non-finite values.
Results may differ from the reference program's by a relative error of at most 0.023.
Values may be sent and summed in bfloat16 or wider, within the bound.
A program may use at most 128 MiB of HBM per device.

```python
import jax
import jax.numpy as jnp
from jax import lax

MODEL_WIDTH = 4096
HEAD_COUNT = 128
HEAD_DIM = 64
STATE_DIM = 128
GROUP_COUNT = 16
CONV_TAPS = 4
LAYER_COUNT = 2
INNER_WIDTH = 8192
VEC_WIDTH = 2048
BATCH_SEQS = 32


def draw_tokens(key, part):
    base_key = jax.random.fold_in(key, 17)
    key_base, key_row = jax.random.split(base_key, 2)
    columns = jnp.exp(jnp.linspace(jnp.log(0.4), jnp.log(2.4), MODEL_WIDTH)).astype(jnp.float32)
    row_scale = jnp.exp(jax.random.uniform(key_row, (BATCH_SEQS, 1), jnp.float32, 0.0, jnp.log(10.0)))
    base = jnp.clip(jax.random.normal(key_base, (BATCH_SEQS, MODEL_WIDTH), jnp.float32), -6.0, 6.0)
    return (0.3 * base * columns[None, :] * row_scale).astype(jnp.bfloat16)


def levels(rng, extent, shards, low, largest):
    factor_of = 1.0
    for axis_at, parts in shards:
        heights = jax.random.uniform(jax.random.fold_in(jax.random.fold_in(rng, 6), axis_at), (parts,), jnp.float32, low / len(shards), largest / len(shards))
        factor_of = factor_of * jnp.repeat(jnp.exp(heights), extent[axis_at] // parts).reshape((-1,) + (1,) * (len(extent) - 1 - axis_at))
    return factor_of


def bell_draw(rng, extent, width, bound, cuts=(), dtype=jnp.bfloat16):
    values = width * jax.random.normal(rng, extent, jnp.float32)
    if cuts:
        values = values * levels(rng, extent, cuts, -0.22, 0.18)
    return jnp.clip(values, -bound, bound).astype(dtype)


def setup_inputs(seed: int = 0, part: int = 0) -> dict:
    key_of = jax.random.split(jax.random.key(seed), 16)
    part_splits = jax.random.split(jax.random.fold_in(key_of[15], part), 16)
    return {
        "tokens": draw_tokens(jax.random.fold_in(jax.random.fold_in(key_of[15], part), 71), part),
        "w_in": bell_draw(key_of[1], (LAYER_COUNT, 2, MODEL_WIDTH, INNER_WIDTH), MODEL_WIDTH ** -0.5, 0.09375, ((2, 4), (3, 4))),
        "w_vec": bell_draw(key_of[2], (LAYER_COUNT, 2, MODEL_WIDTH, VEC_WIDTH), MODEL_WIDTH ** -0.5, 0.09375, ((2, 4), (3, 4))),
        "w_step": bell_draw(key_of[3], (LAYER_COUNT, MODEL_WIDTH, HEAD_COUNT), MODEL_WIDTH ** -0.5, 0.09375, ((1, 4),)),
        "conv_weight": bell_draw(key_of[4], (LAYER_COUNT, CONV_TAPS, INNER_WIDTH), 0.5, 3.0, ((2, 4),)),
        "conv_vec": bell_draw(key_of[5], (LAYER_COUNT, 2, CONV_TAPS, VEC_WIDTH), 0.5, 3.0, ((3, 4),)),
        "conv_state": bell_draw(part_splits[6], (LAYER_COUNT, BATCH_SEQS, CONV_TAPS - 1, INNER_WIDTH), 1.0, 6.0, ((1, 4), (3, 4))),
        "vec_state": bell_draw(part_splits[7], (LAYER_COUNT, 2, BATCH_SEQS, CONV_TAPS - 1, VEC_WIDTH), 1.0, 6.0, ((2, 4), (4, 4))),
        "ssm_state": bell_draw(part_splits[8], (LAYER_COUNT, BATCH_SEQS, HEAD_COUNT, HEAD_DIM, STATE_DIM), 0.5, 4.0, ((1, 4), (2, 4)), jnp.float32),
        "step_bias": jnp.clip(-1.5 + 2.5 * jax.random.uniform(key_of[9], (LAYER_COUNT, HEAD_COUNT), jnp.float32) ** levels(key_of[9], (LAYER_COUNT, HEAD_COUNT), ((1, 4),), -0.2, 0.2), -1.5, 1.0),
        "decay_log": jnp.clip(-4.0 + 5.0 * jax.random.uniform(key_of[10], (LAYER_COUNT, HEAD_COUNT), jnp.float32) ** levels(key_of[10], (LAYER_COUNT, HEAD_COUNT), ((1, 4),), -0.2, 0.2), -4.0, 1.0),
        "skip_gain": jnp.clip(0.5 + 2.5 * jax.random.uniform(key_of[11], (LAYER_COUNT, HEAD_COUNT), jnp.float32) ** levels(key_of[11], (LAYER_COUNT, HEAD_COUNT), ((1, 4),), -0.2, 0.2), 0.5, 3.0),
        "mix_gain": jnp.clip(1.0 + 0.18 * jax.random.normal(key_of[12], (LAYER_COUNT, MODEL_WIDTH), jnp.float32), 0.099609375, 1.8984375).astype(jnp.bfloat16),
        "out_gain": jnp.clip(1.0 + 0.18 * jax.random.normal(key_of[13], (LAYER_COUNT, INNER_WIDTH), jnp.float32), 0.099609375, 1.8984375).astype(jnp.bfloat16),
        "w_out": bell_draw(key_of[14], (LAYER_COUNT, INNER_WIDTH, MODEL_WIDTH), INNER_WIDTH ** -0.5, 0.0625, ((1, 4), (2, 4))),
    }


EPS = 1e-06

def mixer(current, layer, w_in, w_vec, w_step, conv_weight, conv_vec, conv_state, vec_state, ssm_state, step_bias, decay_log, skip_gain, mix_gain, out_gain, w_out):
    batch = current.shape[0]
    xf = current.astype(jnp.float32)
    scale = lax.rsqrt(lax.optimization_barrier(jnp.mean(xf * xf, axis=1)) + EPS)
    scaled_in = (xf * mix_gain[layer].astype(jnp.float32)).astype(jnp.bfloat16)
    proj = jnp.einsum('bd,rdc->brc', scaled_in.astype(jnp.float32), w_in[layer].astype(jnp.float32))
    proj = (proj * scale[:, None, None]).astype(jnp.bfloat16)
    vecs = jnp.einsum('bd,rdc->brc', scaled_in.astype(jnp.float32), w_vec[layer].astype(jnp.float32))
    vecs = (vecs * scale[:, None, None]).astype(jnp.bfloat16)
    step_raw = jnp.dot(scaled_in, w_step[layer], preferred_element_type=jnp.float32) * scale[:, None]
    window = jnp.concatenate([conv_state[layer], proj[:, 1][:, None, :]], axis=1)
    new_conv = window[:, 1:, :]
    values_sum = lax.optimization_barrier(jnp.sum(window.astype(jnp.float32) * conv_weight[layer].astype(jnp.float32)[None, :, :], axis=1))
    fresh = jnp.transpose(vecs, (1, 0, 2))[:, :, None, :]
    vec_window = jnp.concatenate([vec_state[layer], fresh], axis=2)
    new_vec = vec_window[:, :, 1:, :]
    vec_sum = lax.optimization_barrier(jnp.sum(vec_window.astype(jnp.float32) * conv_vec[layer].astype(jnp.float32)[:, None, :, :], axis=2))
    values = jax.nn.silu(values_sum).reshape(batch, HEAD_COUNT, HEAD_DIM)
    vec_act = jax.nn.silu(vec_sum)
    repeat = HEAD_COUNT // GROUP_COUNT
    in_vec = jnp.repeat(vec_act[0].reshape(batch, GROUP_COUNT, STATE_DIM), repeat, axis=1)
    out_vec = jnp.repeat(vec_act[1].reshape(batch, GROUP_COUNT, STATE_DIM), repeat, axis=1)
    step = jax.nn.softplus(step_raw + step_bias[layer][None, :])
    decay = jnp.exp(-step * jnp.exp(decay_log[layer])[None, :])
    state = decay[:, :, None, None] * ssm_state[layer] + (step[:, :, None] * values)[..., None] * in_vec[:, :, None, :]
    read = jnp.einsum('bhpn,bhn->bhp', state, out_vec) + skip_gain[layer][None, :, None] * values
    mixed = read.reshape(batch, INNER_WIDTH) * jax.nn.silu(proj[:, 0].astype(jnp.float32))
    grouped = mixed.reshape(batch, GROUP_COUNT, INNER_WIDTH // GROUP_COUNT)
    grouped = grouped * lax.rsqrt(lax.optimization_barrier(jnp.mean(grouped * grouped, axis=2, keepdims=True)) + EPS)
    normed = (grouped.reshape(batch, INNER_WIDTH) * out_gain[layer].astype(jnp.float32)).astype(jnp.bfloat16)
    result = (xf + jnp.dot(normed, w_out[layer], preferred_element_type=jnp.float32)).astype(jnp.bfloat16)
    return (result, new_conv, new_vec, state)

def reference(tokens, w_in, w_vec, w_step, conv_weight, conv_vec, conv_state, vec_state, ssm_state, step_bias, decay_log, skip_gain, mix_gain, out_gain, w_out):
    current = tokens
    convs = []
    vec_rows = []
    states = []
    for layer in range(LAYER_COUNT):
        current, conv_next, vec_next, state_next = mixer(current, layer, w_in, w_vec, w_step, conv_weight, conv_vec, conv_state, vec_state, ssm_state, step_bias, decay_log, skip_gain, mix_gain, out_gain, w_out)
        convs.append(conv_next)
        vec_rows.append(vec_next)
        states.append(state_next)
    return (current, jnp.stack(convs), jnp.stack(vec_rows), jnp.stack(states))
```

```python
import functools

import jax
import jax.numpy as jnp
from jax import lax
from jax.experimental import pallas as pl
from jax.experimental.pallas import tpu as pltpu
from jax.sharding import PartitionSpec as P

MODEL_WIDTH = 4096
HEAD_COUNT = 128
HEAD_DIM = 64
STATE_DIM = 128
GROUP_COUNT = 16
LAYER_COUNT = 2

EPS = 1e-06
F32 = jnp.float32
BF16 = jnp.bfloat16


def remote(src, dst, send_sem, recv_sem, axis, target):
    return pltpu.make_async_remote_copy(
        src_ref=src,
        dst_ref=dst,
        send_sem=send_sem,
        recv_sem=recv_sem,
        device_id={axis: target},
        device_id_type=pl.DeviceIdType.MESH,
    )


def greet(sizes):
    barrier = pltpu.get_barrier_semaphore()
    count = 0
    for axis, n in sizes:
        me = lax.axis_index(axis)
        for k in range(1, n):
            pl.semaphore_signal(
                barrier,
                inc=1,
                device_id={axis: lax.rem(me + k, n)},
                device_id_type=pl.DeviceIdType.MESH,
            )
            count += 1
    pl.semaphore_wait(barrier, count)


def spread(src, dst, send_sem, recv_sem, axis, n):
    me = lax.axis_index(axis)
    copies = []
    for k in range(1, n):
        copy = remote(src, dst.at[me], send_sem.at[k], recv_sem.at[k], axis, lax.rem(me + k, n))
        copy.start()
        copies.append(copy)
    return copies


def deal(src, dst, send_sem, recv_sem, axis, n, whole=False):
    me = lax.axis_index(axis)
    copies = []
    for k in range(1, n):
        peer = lax.rem(me + k, n)
        copy = remote(
            src if whole else src.at[peer],
            dst.at[k],
            send_sem.at[k],
            recv_sem.at[k],
            axis,
            peer,
        )
        copy.start()
        copies.append(copy)
    return copies


def project(
    layer, ndp, rows_d, lhs, squares, weights, loads, w_step_ref, send, recv, sems, outs
):
    w_in_buf, w_vec_buf = weights
    load_in, load_vec = loads
    send_gate, send_val, send_small = send
    recv_gate, recv_val, recv_small = recv
    proj_ref, vecs_ref, step_ref = outs
    vec_cols = w_vec_buf.shape[2]
    cols = w_in_buf.shape[2]
    heads = w_step_ref.shape[2]
    me = lax.axis_index("dp")

    def put(target, at, acc):
        for p in range(ndp):
            target[p, :, at : at + acc.shape[1]] = acc[p * rows_d : (p + 1) * rows_d].astype(BF16)

    put(send_small, 2 * vec_cols, jnp.dot(lhs, w_step_ref[layer], preferred_element_type=F32))
    put(send_small, 2 * vec_cols + heads, jnp.broadcast_to(squares, (squares.shape[0], 128)))
    load_vec.wait()
    for role in range(2):
        put(send_small, role * vec_cols, jnp.dot(lhs, w_vec_buf[role], preferred_element_type=F32))
    copies = deal(send_small, recv_small, sems[0], sems[1], "dp", ndp)
    block = min(cols, 1024)
    for role in (0, 1):
        target, landing = ((send_gate, recv_gate), (send_val, recv_val))[role]
        load_in[role].wait()
        for at in range(0, cols, block):
            put(
                target,
                at,
                jnp.dot(lhs, w_in_buf[role, :, at : at + block], preferred_element_type=F32),
            )
        copies += deal(target, landing, sems[2 + 2 * role], sems[3 + 2 * role], "dp", ndp)
    for copy in copies:
        copy.wait()

    def total(mine, others):
        acc = mine[me].astype(F32)
        for k in range(1, ndp):
            acc = acc + others[k].astype(F32)
        return acc

    small = total(send_small, recv_small)
    own_sq = small[:, 2 * vec_cols + heads : 2 * vec_cols + heads + 1]
    scale = lax.rsqrt(own_sq * (1.0 / MODEL_WIDTH) + EPS)
    for role in range(2):
        vecs_ref[role] = (small[:, role * vec_cols : (role + 1) * vec_cols] * scale).astype(BF16)
    step_ref[...] = small[:, 2 * vec_cols : 2 * vec_cols + heads] * scale
    proj_ref[0] = (total(send_gate, recv_gate) * scale).astype(BF16)
    proj_ref[1] = (total(send_val, recv_val) * scale).astype(BF16)


def first_kernel(
    ntp, ndp, x_ref, gain_ref, w_step_ref, w_in_ref, w_vec_ref,
    proj_ref, vecs_ref, step_ref, all_ref,
    w_in_buf, w_vec_buf, lhs_buf, landed, send_gate, send_val, send_small,
    recv_gate, recv_val, recv_small, load_sem, ssem_x, rsem_x, *sems,
):
    rows_t = x_ref.shape[0]
    load_vec = pltpu.make_async_copy(w_vec_ref.at[0], w_vec_buf, load_sem.at[0])
    load_vec.start()
    load_in = []
    for role in range(2):
        copy = pltpu.make_async_copy(w_in_ref.at[0, role], w_in_buf.at[role], load_sem.at[1 + role])
        copy.start()
        load_in.append(copy)
    greet((("tp", ntp), ("dp", ndp)))
    copies = spread(x_ref, landed, ssem_x, rsem_x, "tp", ntp)
    landed[lax.axis_index("tp")] = x_ref[...]
    gain = gain_ref[...].astype(F32)[0:1]
    for copy in copies:
        copy.wait()
    squares = []
    for i in range(ntp):
        part = landed[i]
        all_ref[i] = part
        part = part.astype(F32)
        squares.append(jnp.sum(part * part, axis=1, keepdims=True))
        lhs_buf[i * rows_t : (i + 1) * rows_t, :] = part * gain
    squares = jnp.concatenate(squares, axis=0)
    project(
        0, ndp, proj_ref.shape[1], lhs_buf[...].astype(BF16), squares, (w_in_buf, w_vec_buf),
        (load_in, load_vec), w_step_ref, (send_gate, send_val, send_small),
        (recv_gate, recv_val, recv_small), sems, (proj_ref, vecs_ref, step_ref),
    )


def gather_normed(ndp, normed_ref, held, lhs_out, send_sem, recv_sem):
    rows_d = normed_ref.shape[0]
    copies = spread(normed_ref, held, send_sem, recv_sem, "dp", ndp)
    held[lax.axis_index("dp")] = normed_ref[...]
    for copy in copies:
        copy.wait()
    for i in range(ndp):
        lhs_out[i * rows_d : (i + 1) * rows_d, :] = held[i].astype(F32)
    return lhs_out[...].astype(BF16)


def middle_kernel(
    layer, ntp, ndp, normed_ref, old_ref, gain_ref, w_step_ref, w_out_ref, w_in_ref, w_vec_ref,
    proj_ref, vecs_ref, step_ref, all_ref,
    w_out_buf, w_in_buf, w_vec_buf, lhs_out, lhs_buf, held, part_out, parts_in,
    send_gate, send_val, send_small, recv_gate, recv_val, recv_small,
    load_sem, ssem_n, rsem_n, ssem_o, rsem_o, *sems,
):
    rows_t = old_ref.shape[1]
    load_out = pltpu.make_async_copy(w_out_ref.at[layer - 1], w_out_buf, load_sem.at[3])
    load_out.start()
    load_vec = pltpu.make_async_copy(w_vec_ref.at[layer], w_vec_buf, load_sem.at[0])
    load_vec.start()
    load_in = []
    for role in range(2):
        copy = pltpu.make_async_copy(
            w_in_ref.at[layer, role], w_in_buf.at[role], load_sem.at[1 + role]
        )
        copy.start()
        load_in.append(copy)
    greet((("tp", ntp), ("dp", ndp)))
    lhs = gather_normed(ndp, normed_ref, held, lhs_out, ssem_n, rsem_n)
    gain = gain_ref[...].astype(F32)[layer : layer + 1]
    load_out.wait()
    part_out[...] = jnp.dot(lhs, w_out_buf[...], preferred_element_type=F32).astype(BF16)
    copies = deal(part_out, parts_in, ssem_o, rsem_o, "tp", ntp, whole=True)
    for copy in copies:
        copy.wait()
    acc = part_out[...].astype(F32)
    for k in range(1, ntp):
        acc = acc + parts_in[k].astype(F32)
    squares = []
    for i in range(ntp):
        part = (old_ref[i].astype(F32) + acc[i * rows_t : (i + 1) * rows_t]).astype(BF16)
        all_ref[i] = part
        part = part.astype(F32)
        squares.append(jnp.sum(part * part, axis=1, keepdims=True))
        lhs_buf[i * rows_t : (i + 1) * rows_t, :] = part * gain
    squares = jnp.concatenate(squares, axis=0)
    project(
        layer, ndp, proj_ref.shape[1], lhs_buf[...].astype(BF16), squares, (w_in_buf, w_vec_buf),
        (load_in, load_vec), w_step_ref, (send_gate, send_val, send_small),
        (recv_gate, recv_val, recv_small), sems, (proj_ref, vecs_ref, step_ref),
    )


def last_kernel(
    layer, ntp, ndp, normed_ref, old_ref, w_out_ref, out_ref,
    w_out_buf, lhs_out, held, send_out, recv_out, load_sem, ssem_n, rsem_n, ssem_o, rsem_o,
):
    rows_t = old_ref.shape[1]
    load_out = pltpu.make_async_copy(w_out_ref.at[layer], w_out_buf, load_sem)
    load_out.start()
    greet((("tp", ntp), ("dp", ndp)))
    lhs = gather_normed(ndp, normed_ref, held, lhs_out, ssem_n, rsem_n)
    load_out.wait()
    acc = jnp.dot(lhs, w_out_buf[...], preferred_element_type=F32)
    for i in range(ntp):
        send_out[i] = acc[i * rows_t : (i + 1) * rows_t].astype(BF16)
    me = lax.axis_index("tp")
    copies = deal(send_out, recv_out, ssem_o, rsem_o, "tp", ntp)
    for copy in copies:
        copy.wait()
    acc = send_out[me].astype(F32)
    for k in range(1, ntp):
        acc = acc + recv_out[k].astype(F32)
    out_ref[...] = (old_ref[me].astype(F32) + acc).astype(BF16)


VMEM = pl.BlockSpec(memory_space=pltpu.VMEM)
HBM = pl.BlockSpec(memory_space=pl.ANY)


def sizes_of(tokens, w_in, w_vec, w_step, ntp, ndp):
    rows_t, width = tokens.shape
    batch = rows_t * ntp
    return rows_t, width, batch, batch // ndp, w_in.shape[3], w_vec.shape[3], w_step.shape[2]


def dma(n):
    return pltpu.SemaphoreType.DMA((n,))


def mixer_scratch(width, cols, vcols, heads, rows_d, ndp):
    small = 2 * vcols + heads + 128
    return [
        pltpu.VMEM((2, width, cols), BF16),
        pltpu.VMEM((2, width, vcols), BF16),
    ], [
        pltpu.VMEM((ndp, rows_d, cols), BF16),
        pltpu.VMEM((ndp, rows_d, cols), BF16),
        pltpu.VMEM((ndp, rows_d, small), BF16),
        pltpu.VMEM((ndp, rows_d, cols), BF16),
        pltpu.VMEM((ndp, rows_d, cols), BF16),
        pltpu.VMEM((ndp, rows_d, small), BF16),
    ]


def first_call(ntp, ndp, tokens, mix_gain, w_step, w_in, w_vec):
    rows_t, width, batch, rows_d, cols, vcols, heads = sizes_of(
        tokens, w_in, w_vec, w_step, ntp, ndp
    )
    bufs, wires = mixer_scratch(width, cols, vcols, heads, rows_d, ndp)
    return pl.pallas_call(
        functools.partial(first_kernel, ntp, ndp),
        out_shape=(
            jax.ShapeDtypeStruct((2, rows_d, cols), BF16),
            jax.ShapeDtypeStruct((2, rows_d, vcols), BF16),
            jax.ShapeDtypeStruct((rows_d, heads), F32),
            jax.ShapeDtypeStruct((ntp, rows_t, width), BF16),
        ),
        in_specs=[VMEM, VMEM, VMEM, HBM, HBM],
        out_specs=(VMEM,) * 4,
        scratch_shapes=bufs
        + [pltpu.VMEM((batch, width), F32), pltpu.VMEM((ntp, rows_t, width), BF16)]
        + wires
        + [dma(3), dma(ntp), dma(ntp)]
        + [dma(ndp)] * 6,
        compiler_params=pltpu.CompilerParams(collective_id=0, has_side_effects=True),
    )(tokens, mix_gain, w_step, w_in, w_vec)


def middle_call(layer, ntp, ndp, tokens, normed, old, mix_gain, w_step, w_out, w_in, w_vec):
    rows_t, width, batch, rows_d, cols, vcols, heads = sizes_of(
        tokens, w_in, w_vec, w_step, ntp, ndp
    )
    bufs, wires = mixer_scratch(width, cols, vcols, heads, rows_d, ndp)
    return pl.pallas_call(
        functools.partial(middle_kernel, layer, ntp, ndp),
        out_shape=(
            jax.ShapeDtypeStruct((2, rows_d, cols), BF16),
            jax.ShapeDtypeStruct((2, rows_d, vcols), BF16),
            jax.ShapeDtypeStruct((rows_d, heads), F32),
            jax.ShapeDtypeStruct((ntp, rows_t, width), BF16),
        ),
        in_specs=[VMEM, VMEM, VMEM, VMEM, HBM, HBM, HBM],
        out_specs=(VMEM,) * 4,
        scratch_shapes=[pltpu.VMEM((cols, width), BF16)]
        + bufs
        + [
            pltpu.VMEM((batch, cols), F32),
            pltpu.VMEM((batch, width), F32),
            pltpu.VMEM((ndp, rows_d, cols), BF16),
            pltpu.VMEM((batch, width), BF16),
            pltpu.VMEM((ntp, batch, width), BF16),
        ]
        + wires
        + [dma(4), dma(ndp), dma(ndp), dma(ntp), dma(ntp)]
        + [dma(ndp)] * 6,
        compiler_params=pltpu.CompilerParams(collective_id=layer, has_side_effects=True),
    )(normed, old, mix_gain, w_step, w_out, w_in, w_vec)


def last_call(layer, ntp, ndp, normed, old, w_out):
    _, rows_t, width = old.shape
    rows_d, cols = normed.shape
    batch = rows_t * ntp
    return pl.pallas_call(
        functools.partial(last_kernel, layer, ntp, ndp),
        out_shape=jax.ShapeDtypeStruct((rows_t, width), BF16),
        in_specs=[VMEM, VMEM, HBM],
        out_specs=VMEM,
        scratch_shapes=[
            pltpu.VMEM((cols, width), BF16),
            pltpu.VMEM((batch, cols), F32),
            pltpu.VMEM((ndp, rows_d, cols), BF16),
            pltpu.VMEM((ntp, rows_t, width), BF16),
            pltpu.VMEM((ntp, rows_t, width), BF16),
            pltpu.SemaphoreType.DMA,
            dma(ndp), dma(ndp), dma(ntp), dma(ntp),
        ],
        compiler_params=pltpu.CompilerParams(collective_id=layer + 1, has_side_effects=True),
    )(normed, old, w_out)


def head_step(
    layer, proj, vecs, step_all, conv_weight, conv_vec, conv_state, vec_state, ssm_state,
    step_bias, decay_log, skip_gain, out_gain,
):
    local_rows, columns = proj.shape[1:]
    vec_columns = vecs.shape[2]
    local_heads = ssm_state.shape[2]
    head_start = lax.axis_index("tp") * local_heads
    step_raw = lax.dynamic_slice_in_dim(step_all, head_start, local_heads, 1)
    window = jnp.concatenate([conv_state[layer], proj[1][:, None, :]], axis=1)
    new_conv = window[:, 1:, :]
    values_sum = jnp.sum(
        window.astype(jnp.float32) * conv_weight[layer].astype(jnp.float32)[None, :, :], axis=1
    )
    fresh = vecs[:, :, None, :]
    vec_window = jnp.concatenate([vec_state[layer], fresh], axis=2)
    new_vec = vec_window[:, :, 1:, :]
    vec_sum = jnp.sum(
        vec_window.astype(jnp.float32) * conv_vec[layer].astype(jnp.float32)[:, None, :, :], axis=2
    )
    values = jax.nn.silu(values_sum).reshape(local_rows, local_heads, HEAD_DIM)
    vec_act = jax.nn.silu(vec_sum)
    local_groups = vec_columns // STATE_DIM
    repeat = HEAD_COUNT // GROUP_COUNT
    in_vec = jnp.repeat(vec_act[0].reshape(local_rows, local_groups, STATE_DIM), repeat, axis=1)
    out_vec = jnp.repeat(vec_act[1].reshape(local_rows, local_groups, STATE_DIM), repeat, axis=1)
    step = jax.nn.softplus(step_raw + step_bias[layer][None, :])
    decay = jnp.exp(-step * jnp.exp(decay_log[layer])[None, :])
    state = (
        decay[:, :, None, None] * ssm_state[layer]
        + (step[:, :, None] * values)[..., None] * in_vec[:, :, None, :]
    )
    read = jnp.einsum("bhpn,bhn->bhp", state, out_vec) + skip_gain[layer][None, :, None] * values
    mixed = read.reshape(local_rows, columns) * jax.nn.silu(proj[0].astype(jnp.float32))
    grouped = mixed.reshape(local_rows, local_groups, columns // local_groups)
    grouped = grouped * lax.rsqrt(jnp.mean(grouped * grouped, axis=2, keepdims=True) + EPS)
    normed = (grouped.reshape(local_rows, columns) * out_gain[layer].astype(jnp.float32)).astype(
        jnp.bfloat16
    )
    return (normed, new_conv, new_vec, state)


def shards(
    ntp,
    ndp,
    tokens,
    w_in,
    w_vec,
    w_step,
    conv_weight,
    conv_vec,
    conv_state,
    vec_state,
    ssm_state,
    step_bias,
    decay_log,
    skip_gain,
    mix_gain,
    out_gain,
    w_out,
):
    convs = []
    vec_rows = []
    states = []
    for layer in range(LAYER_COUNT):
        if layer == 0:
            proj, vecs, step_all, rows = first_call(
                ntp, ndp, tokens, mix_gain, w_step, w_in, w_vec
            )
        else:
            proj, vecs, step_all, rows = middle_call(
                layer, ntp, ndp, tokens, normed, rows, mix_gain, w_step, w_out, w_in, w_vec
            )
        normed, conv_next, vec_next, state_next = head_step(
            layer, proj, vecs, step_all, conv_weight, conv_vec, conv_state, vec_state,
            ssm_state, step_bias, decay_log, skip_gain, out_gain,
        )
        convs.append(conv_next)
        vec_rows.append(vec_next)
        states.append(state_next)
    current = last_call(LAYER_COUNT - 1, ntp, ndp, normed, rows, w_out)
    return (current, jnp.stack(convs), jnp.stack(vec_rows), jnp.stack(states))


def solution(mesh):
    placed = (
        P(("grp", "tp"), "dp"),
        P(None, None, "dp", "tp"),
        P(None, None, "dp", "tp"),
        P(None, "dp", None),
        P(None, None, "tp"),
        P(None, None, None, "tp"),
        P(None, ("grp", "dp"), None, "tp"),
        P(None, None, ("grp", "dp"), None, "tp"),
        P(None, ("grp", "dp"), "tp", None, None),
        P(None, "tp"),
        P(None, "tp"),
        P(None, "tp"),
        P(None, "dp"),
        P(None, "tp"),
        P(None, "tp", "dp"),
    )
    return jax.shard_map(
        functools.partial(shards, mesh.shape["tp"], mesh.shape["dp"]),
        mesh=mesh,
        in_specs=placed,
        out_specs=(
            P(("grp", "tp"), "dp"),
            P(None, ("grp", "dp"), None, "tp"),
            P(None, None, ("grp", "dp"), None, "tp"),
            P(None, ("grp", "dp"), "tp", None, None),
        ),
        check_vma=False,
    )
```

```python
import functools

import jax
import jax.numpy as jnp
from jax import lax
from jax.experimental import pallas as pl
from jax.experimental.pallas import tpu as pltpu
from jax.sharding import PartitionSpec as P

MODEL_WIDTH = 4096
HEAD_COUNT = 128
HEAD_DIM = 64
STATE_DIM = 128
GROUP_COUNT = 16
LAYER_COUNT = 2

EPS = 1e-06
F32 = jnp.float32
BF16 = jnp.bfloat16


def remote(src, dst, send_sem, recv_sem, axis, target):
    return pltpu.make_async_remote_copy(
        src_ref=src,
        dst_ref=dst,
        send_sem=send_sem,
        recv_sem=recv_sem,
        device_id={axis: target},
        device_id_type=pl.DeviceIdType.MESH,
    )


def greet(sizes):
    barrier = pltpu.get_barrier_semaphore()
    count = 0
    for axis, n in sizes:
        me = lax.axis_index(axis)
        for k in range(1, n):
            pl.semaphore_signal(
                barrier,
                inc=1,
                device_id={axis: lax.rem(me + k, n)},
                device_id_type=pl.DeviceIdType.MESH,
            )
            count += 1
    pl.semaphore_wait(barrier, count)


def spread(src, dst, send_sem, recv_sem, axis, n):
    me = lax.axis_index(axis)
    copies = []
    for k in range(1, n):
        copy = remote(src, dst.at[me], send_sem.at[k], recv_sem.at[k], axis, lax.rem(me + k, n))
        copy.start()
        copies.append(copy)
    return copies


def deal(src, dst, send_sem, recv_sem, axis, n, whole=False):
    me = lax.axis_index(axis)
    copies = []
    for k in range(1, n):
        peer = lax.rem(me + k, n)
        copy = remote(
            src if whole else src.at[peer],
            dst.at[k],
            send_sem.at[k],
            recv_sem.at[k],
            axis,
            peer,
        )
        copy.start()
        copies.append(copy)
    return copies


def project(
    layer, ndp, rows_d, lhs, squares, weights, loads, w_step_ref, send, recv, sems, outs
):
    w_in_buf, w_vec_buf = weights
    load_in, load_vec = loads
    send_gate, send_val, send_small = send
    recv_gate, recv_val, recv_small = recv
    proj_ref, vecs_ref, step_ref = outs
    vec_cols = w_vec_buf.shape[2]
    cols = w_in_buf.shape[2]
    heads = w_step_ref.shape[2]
    me = lax.axis_index("dp")

    def put(target, at, acc):
        for p in range(ndp):
            target[p, :, at : at + acc.shape[1]] = acc[p * rows_d : (p + 1) * rows_d].astype(BF16)

    put(send_small, 2 * vec_cols, jnp.dot(lhs, w_step_ref[layer], preferred_element_type=F32))
    put(send_small, 2 * vec_cols + heads, jnp.broadcast_to(squares, (squares.shape[0], 128)))
    load_vec.wait()
    for role in range(2):
        put(send_small, role * vec_cols, jnp.dot(lhs, w_vec_buf[role], preferred_element_type=F32))
    copies = deal(send_small, recv_small, sems[0], sems[1], "dp", ndp)
    block = min(cols, 1024)
    for role in (0, 1):
        target, landing = ((send_gate, recv_gate), (send_val, recv_val))[role]
        load_in[role].wait()
        for at in range(0, cols, block):
            put(
                target,
                at,
                jnp.dot(lhs, w_in_buf[role, :, at : at + block], preferred_element_type=F32),
            )
        copies += deal(target, landing, sems[2 + 2 * role], sems[3 + 2 * role], "dp", ndp)
    for copy in copies:
        copy.wait()

    def total(mine, others):
        acc = mine[me].astype(F32)
        for k in range(1, ndp):
            acc = acc + others[k].astype(F32)
        return acc

    small = total(send_small, recv_small)
    own_sq = small[:, 2 * vec_cols + heads : 2 * vec_cols + heads + 1]
    scale = lax.rsqrt(own_sq * (1.0 / MODEL_WIDTH) + EPS)
    for role in range(2):
        vecs_ref[role] = (small[:, role * vec_cols : (role + 1) * vec_cols] * scale).astype(BF16)
    step_ref[...] = small[:, 2 * vec_cols : 2 * vec_cols + heads] * scale
    proj_ref[0] = (total(send_gate, recv_gate) * scale).astype(BF16)
    proj_ref[1] = (total(send_val, recv_val) * scale).astype(BF16)


def first_kernel(
    ntp, ndp, x_ref, gain_ref, w_step_ref, w_in_ref, w_vec_ref,
    proj_ref, vecs_ref, step_ref, all_ref,
    w_in_buf, w_vec_buf, lhs_buf, landed, send_gate, send_val, send_small,
    recv_gate, recv_val, recv_small, load_sem, ssem_x, rsem_x, *sems,
):
    rows_t = x_ref.shape[0]
    load_vec = pltpu.make_async_copy(w_vec_ref.at[0], w_vec_buf, load_sem.at[0])
    load_vec.start()
    load_in = []
    for role in range(2):
        copy = pltpu.make_async_copy(w_in_ref.at[0, role], w_in_buf.at[role], load_sem.at[1 + role])
        copy.start()
        load_in.append(copy)
    greet((("tp", ntp), ("dp", ndp)))
    copies = spread(x_ref, landed, ssem_x, rsem_x, "tp", ntp)
    landed[lax.axis_index("tp")] = x_ref[...]
    gain = gain_ref[...].astype(F32)[0:1]
    for copy in copies:
        copy.wait()
    squares = []
    for i in range(ntp):
        part = landed[i]
        all_ref[i] = part
        part = part.astype(F32)
        squares.append(jnp.sum(part * part, axis=1, keepdims=True))
        lhs_buf[i * rows_t : (i + 1) * rows_t, :] = part * gain
    squares = jnp.concatenate(squares, axis=0)
    project(
        0, ndp, proj_ref.shape[1], lhs_buf[...].astype(BF16), squares, (w_in_buf, w_vec_buf),
        (load_in, load_vec), w_step_ref, (send_gate, send_val, send_small),
        (recv_gate, recv_val, recv_small), sems, (proj_ref, vecs_ref, step_ref),
    )


def gather_normed(ndp, normed_ref, held, lhs_out, send_sem, recv_sem):
    rows_d = normed_ref.shape[0]
    copies = spread(normed_ref, held, send_sem, recv_sem, "dp", ndp)
    held[lax.axis_index("dp")] = normed_ref[...]
    for copy in copies:
        copy.wait()
    for i in range(ndp):
        lhs_out[i * rows_d : (i + 1) * rows_d, :] = held[i].astype(F32)
    return lhs_out[...].astype(BF16)


def middle_kernel(
    layer, ntp, ndp, normed_ref, old_ref, gain_ref, w_step_ref, w_out_ref, w_in_ref, w_vec_ref,
    proj_ref, vecs_ref, step_ref, all_ref,
    w_out_buf, w_in_buf, w_vec_buf, lhs_out, lhs_buf, held, part_out, parts_in,
    send_gate, send_val, send_small, recv_gate, recv_val, recv_small,
    load_sem, ssem_n, rsem_n, ssem_o, rsem_o, *sems,
):
    rows_t = old_ref.shape[1]
    load_out = pltpu.make_async_copy(w_out_ref.at[layer - 1], w_out_buf, load_sem.at[3])
    load_out.start()
    load_vec = pltpu.make_async_copy(w_vec_ref.at[layer], w_vec_buf, load_sem.at[0])
    load_vec.start()
    load_in = []
    for role in range(2):
        copy = pltpu.make_async_copy(
            w_in_ref.at[layer, role], w_in_buf.at[role], load_sem.at[1 + role]
        )
        copy.start()
        load_in.append(copy)
    greet((("tp", ntp), ("dp", ndp)))
    lhs = gather_normed(ndp, normed_ref, held, lhs_out, ssem_n, rsem_n)
    gain = gain_ref[...].astype(F32)[layer : layer + 1]
    load_out.wait()
    part_out[...] = jnp.dot(lhs, w_out_buf[...], preferred_element_type=F32).astype(BF16)
    copies = deal(part_out, parts_in, ssem_o, rsem_o, "tp", ntp, whole=True)
    for copy in copies:
        copy.wait()
    acc = part_out[...].astype(F32)
    for k in range(1, ntp):
        acc = acc + parts_in[k].astype(F32)
    squares = []
    for i in range(ntp):
        part = (old_ref[i].astype(F32) + acc[i * rows_t : (i + 1) * rows_t]).astype(BF16)
        all_ref[i] = part
        part = part.astype(F32)
        squares.append(jnp.sum(part * part, axis=1, keepdims=True))
        lhs_buf[i * rows_t : (i + 1) * rows_t, :] = part * gain
    squares = jnp.concatenate(squares, axis=0)
    project(
        layer, ndp, proj_ref.shape[1], lhs_buf[...].astype(BF16), squares, (w_in_buf, w_vec_buf),
        (load_in, load_vec), w_step_ref, (send_gate, send_val, send_small),
        (recv_gate, recv_val, recv_small), sems, (proj_ref, vecs_ref, step_ref),
    )


def last_kernel(
    layer, ntp, ndp, normed_ref, old_ref, w_out_ref, out_ref,
    w_out_buf, lhs_out, held, send_out, recv_out, load_sem, ssem_n, rsem_n, ssem_o, rsem_o,
):
    rows_t = old_ref.shape[1]
    load_out = pltpu.make_async_copy(w_out_ref.at[layer], w_out_buf, load_sem)
    load_out.start()
    greet((("tp", ntp), ("dp", ndp)))
    lhs = gather_normed(ndp, normed_ref, held, lhs_out, ssem_n, rsem_n)
    load_out.wait()
    acc = jnp.dot(lhs, w_out_buf[...], preferred_element_type=F32)
    for i in range(ntp):
        send_out[i] = acc[i * rows_t : (i + 1) * rows_t].astype(BF16)
    me = lax.axis_index("tp")
    copies = deal(send_out, recv_out, ssem_o, rsem_o, "tp", ntp)
    for copy in copies:
        copy.wait()
    acc = send_out[me].astype(F32)
    for k in range(1, ntp):
        acc = acc + recv_out[k].astype(F32)
    out_ref[...] = (old_ref[me].astype(F32) + acc).astype(BF16)


VMEM = pl.BlockSpec(memory_space=pltpu.VMEM)
HBM = pl.BlockSpec(memory_space=pl.ANY)


def sizes_of(tokens, w_in, w_vec, w_step, ntp, ndp):
    rows_t, width = tokens.shape
    batch = rows_t * ntp
    return rows_t, width, batch, batch // ndp, w_in.shape[3], w_vec.shape[3], w_step.shape[2]


def dma(n):
    return pltpu.SemaphoreType.DMA((n,))


def mixer_scratch(width, cols, vcols, heads, rows_d, ndp):
    small = 2 * vcols + heads + 128
    return [
        pltpu.VMEM((2, width, cols), BF16),
        pltpu.VMEM((2, width, vcols), BF16),
    ], [
        pltpu.VMEM((ndp, rows_d, cols), BF16),
        pltpu.VMEM((ndp, rows_d, cols), BF16),
        pltpu.VMEM((ndp, rows_d, small), BF16),
        pltpu.VMEM((ndp, rows_d, cols), BF16),
        pltpu.VMEM((ndp, rows_d, cols), BF16),
        pltpu.VMEM((ndp, rows_d, small), BF16),
    ]


def first_call(ntp, ndp, tokens, mix_gain, w_step, w_in, w_vec):
    rows_t, width, batch, rows_d, cols, vcols, heads = sizes_of(
        tokens, w_in, w_vec, w_step, ntp, ndp
    )
    bufs, wires = mixer_scratch(width, cols, vcols, heads, rows_d, ndp)
    return pl.pallas_call(
        functools.partial(first_kernel, ntp, ndp),
        out_shape=(
            jax.ShapeDtypeStruct((2, rows_d, cols), BF16),
            jax.ShapeDtypeStruct((2, rows_d, vcols), BF16),
            jax.ShapeDtypeStruct((rows_d, heads), F32),
            jax.ShapeDtypeStruct((ntp, rows_t, width), BF16),
        ),
        in_specs=[VMEM, VMEM, VMEM, HBM, HBM],
        out_specs=(VMEM,) * 4,
        scratch_shapes=bufs
        + [pltpu.VMEM((batch, width), F32), pltpu.VMEM((ntp, rows_t, width), BF16)]
        + wires
        + [dma(3), dma(ntp), dma(ntp)]
        + [dma(ndp)] * 6,
        compiler_params=pltpu.CompilerParams(collective_id=0, has_side_effects=True),
    )(tokens, mix_gain, w_step, w_in, w_vec)


def middle_call(layer, ntp, ndp, tokens, normed, old, mix_gain, w_step, w_out, w_in, w_vec):
    rows_t, width, batch, rows_d, cols, vcols, heads = sizes_of(
        tokens, w_in, w_vec, w_step, ntp, ndp
    )
    bufs, wires = mixer_scratch(width, cols, vcols, heads, rows_d, ndp)
    return pl.pallas_call(
        functools.partial(middle_kernel, layer, ntp, ndp),
        out_shape=(
            jax.ShapeDtypeStruct((2, rows_d, cols), BF16),
            jax.ShapeDtypeStruct((2, rows_d, vcols), BF16),
            jax.ShapeDtypeStruct((rows_d, heads), F32),
            jax.ShapeDtypeStruct((ntp, rows_t, width), BF16),
        ),
        in_specs=[VMEM, VMEM, VMEM, VMEM, HBM, HBM, HBM],
        out_specs=(VMEM,) * 4,
        scratch_shapes=[pltpu.VMEM((cols, width), BF16)]
        + bufs
        + [
            pltpu.VMEM((batch, cols), F32),
            pltpu.VMEM((batch, width), F32),
            pltpu.VMEM((ndp, rows_d, cols), BF16),
            pltpu.VMEM((batch, width), BF16),
            pltpu.VMEM((ntp, batch, width), BF16),
        ]
        + wires
        + [dma(4), dma(ndp), dma(ndp), dma(ntp), dma(ntp)]
        + [dma(ndp)] * 6,
        compiler_params=pltpu.CompilerParams(collective_id=layer, has_side_effects=True),
    )(normed, old, mix_gain, w_step, w_out, w_in, w_vec)


def last_call(layer, ntp, ndp, normed, old, w_out):
    _, rows_t, width = old.shape
    rows_d, cols = normed.shape
    batch = rows_t * ntp
    return pl.pallas_call(
        functools.partial(last_kernel, layer, ntp, ndp),
        out_shape=jax.ShapeDtypeStruct((rows_t, width), BF16),
        in_specs=[VMEM, VMEM, HBM],
        out_specs=VMEM,
        scratch_shapes=[
            pltpu.VMEM((cols, width), BF16),
            pltpu.VMEM((batch, cols), F32),
            pltpu.VMEM((ndp, rows_d, cols), BF16),
            pltpu.VMEM((ntp, rows_t, width), BF16),
            pltpu.VMEM((ntp, rows_t, width), BF16),
            pltpu.SemaphoreType.DMA,
            dma(ndp), dma(ndp), dma(ntp), dma(ntp),
        ],
        compiler_params=pltpu.CompilerParams(collective_id=layer + 1, has_side_effects=True),
    )(normed, old, w_out)


def head_step(
    layer, proj, vecs, step_all, conv_weight, conv_vec, conv_state, vec_state, ssm_state,
    step_bias, decay_log, skip_gain, out_gain,
):
    local_rows, columns = proj.shape[1:]
    vec_columns = vecs.shape[2]
    local_heads = ssm_state.shape[2]
    head_start = lax.axis_index("tp") * local_heads
    step_raw = lax.dynamic_slice_in_dim(step_all, head_start, local_heads, 1)
    window = jnp.concatenate([conv_state[layer], proj[1][:, None, :]], axis=1)
    new_conv = window[:, 1:, :]
    values_sum = jnp.sum(
        window.astype(jnp.float32) * conv_weight[layer].astype(jnp.float32)[None, :, :], axis=1
    )
    fresh = vecs[:, :, None, :]
    vec_window = jnp.concatenate([vec_state[layer], fresh], axis=2)
    new_vec = vec_window[:, :, 1:, :]
    vec_sum = jnp.sum(
        vec_window.astype(jnp.float32) * conv_vec[layer].astype(jnp.float32)[:, None, :, :], axis=2
    )
    values = jax.nn.silu(values_sum).reshape(local_rows, local_heads, HEAD_DIM)
    vec_act = jax.nn.silu(vec_sum)
    local_groups = vec_columns // STATE_DIM
    repeat = HEAD_COUNT // GROUP_COUNT
    in_vec = jnp.repeat(vec_act[0].reshape(local_rows, local_groups, STATE_DIM), repeat, axis=1)
    out_vec = jnp.repeat(vec_act[1].reshape(local_rows, local_groups, STATE_DIM), repeat, axis=1)
    step = jax.nn.softplus(step_raw + step_bias[layer][None, :])
    decay = jnp.exp(-step * jnp.exp(decay_log[layer])[None, :])
    state = (
        decay[:, :, None, None] * ssm_state[layer]
        + (step[:, :, None] * values)[..., None] * in_vec[:, :, None, :]
    )
    read = jnp.einsum("bhpn,bhn->bhp", state, out_vec) + skip_gain[layer][None, :, None] * values
    mixed = read.reshape(local_rows, columns) * jax.nn.silu(proj[0].astype(jnp.float32))
    grouped = mixed.reshape(local_rows, local_groups, columns // local_groups)
    grouped = grouped * lax.rsqrt(jnp.mean(grouped * grouped, axis=2, keepdims=True) + EPS)
    normed = (grouped.reshape(local_rows, columns) * out_gain[layer].astype(jnp.float32)).astype(
        jnp.bfloat16
    )
    return (normed, new_conv, new_vec, (decay, step[:, :, None] * values, in_vec))


def shards(
    ntp,
    ndp,
    tokens,
    w_in,
    w_vec,
    w_step,
    conv_weight,
    conv_vec,
    conv_state,
    vec_state,
    ssm_state,
    step_bias,
    decay_log,
    skip_gain,
    mix_gain,
    out_gain,
    w_out,
):
    convs = []
    vec_rows = []
    states = []
    for layer in range(LAYER_COUNT):
        if layer == 0:
            proj, vecs, step_all, rows = first_call(
                ntp, ndp, tokens, mix_gain, w_step, w_in, w_vec
            )
        else:
            proj, vecs, step_all, rows = middle_call(
                layer, ntp, ndp, tokens, normed, rows, mix_gain, w_step, w_out, w_in, w_vec
            )
        normed, conv_next, vec_next, state_next = head_step(
            layer, proj, vecs, step_all, conv_weight, conv_vec, conv_state, vec_state,
            ssm_state, step_bias, decay_log, skip_gain, out_gain,
        )
        convs.append(conv_next)
        vec_rows.append(vec_next)
        states.append(state_next)
    current = last_call(LAYER_COUNT - 1, ntp, ndp, normed, rows, w_out)
    decays, drives, inputs = (jnp.stack(parts) for parts in zip(*states))
    new_ssm = (
        decays[..., None, None] * ssm_state + drives[..., None] * inputs[:, :, :, None, :]
    )
    return (current, jnp.stack(convs), jnp.stack(vec_rows), new_ssm)


def solution(mesh):
    placed = (
        P(("grp", "tp"), "dp"),
        P(None, None, "dp", "tp"),
        P(None, None, "dp", "tp"),
        P(None, "dp", None),
        P(None, None, "tp"),
        P(None, None, None, "tp"),
        P(None, ("grp", "dp"), None, "tp"),
        P(None, None, ("grp", "dp"), None, "tp"),
        P(None, ("grp", "dp"), "tp", None, None),
        P(None, "tp"),
        P(None, "tp"),
        P(None, "tp"),
        P(None, "dp"),
        P(None, "tp"),
        P(None, "tp", "dp"),
    )
    return jax.shard_map(
        functools.partial(shards, mesh.shape["tp"], mesh.shape["dp"]),
        mesh=mesh,
        in_specs=placed,
        out_specs=(
            P(("grp", "tp"), "dp"),
            P(None, ("grp", "dp"), None, "tp"),
            P(None, None, ("grp", "dp"), None, "tp"),
            P(None, ("grp", "dp"), "tp", None, None),
        ),
        check_vma=False,
    )
```

```python
import functools

import jax
import jax.numpy as jnp
from jax import lax
from jax.experimental import pallas as pl
from jax.experimental.pallas import tpu as pltpu
from jax.sharding import PartitionSpec as P

MODEL_WIDTH = 4096
HEAD_COUNT = 128
HEAD_DIM = 64
STATE_DIM = 128
GROUP_COUNT = 16
LAYER_COUNT = 2

EPS = 1e-06
F32 = jnp.float32
BF16 = jnp.bfloat16


def remote(src, dst, send_sem, recv_sem, axis, target):
    return pltpu.make_async_remote_copy(
        src_ref=src,
        dst_ref=dst,
        send_sem=send_sem,
        recv_sem=recv_sem,
        device_id={axis: target},
        device_id_type=pl.DeviceIdType.MESH,
    )


def greet(sizes):
    barrier = pltpu.get_barrier_semaphore()
    count = 0
    for axis, n in sizes:
        me = lax.axis_index(axis)
        for k in range(1, n):
            pl.semaphore_signal(
                barrier,
                inc=1,
                device_id={axis: lax.rem(me + k, n)},
                device_id_type=pl.DeviceIdType.MESH,
            )
            count += 1
    pl.semaphore_wait(barrier, count)


def spread(src, dst, send_sem, recv_sem, axis, n):
    me = lax.axis_index(axis)
    copies = []
    for k in range(1, n):
        copy = remote(src, dst.at[me], send_sem.at[k], recv_sem.at[k], axis, lax.rem(me + k, n))
        copy.start()
        copies.append(copy)
    return copies


def deal(src, dst, send_sem, recv_sem, axis, n, whole=False):
    me = lax.axis_index(axis)
    copies = []
    for k in range(1, n):
        peer = lax.rem(me + k, n)
        copy = remote(
            src if whole else src.at[peer],
            dst.at[k],
            send_sem.at[k],
            recv_sem.at[k],
            axis,
            peer,
        )
        copy.start()
        copies.append(copy)
    return copies


def project(
    layer, ndp, rows_d, lhs, squares, weights, loads, w_step_ref, send, recv, sems, outs
):
    w_in_buf, w_vec_buf = weights
    load_in, load_vec = loads
    send_gate, send_val, send_small = send
    recv_gate, recv_val, recv_small = recv
    proj_ref, vecs_ref, step_ref = outs
    vec_cols = w_vec_buf.shape[2]
    cols = w_in_buf.shape[2]
    heads = w_step_ref.shape[2]
    me = lax.axis_index("dp")

    def put(target, at, acc):
        for p in range(ndp):
            target[p, :, at : at + acc.shape[1]] = acc[p * rows_d : (p + 1) * rows_d].astype(BF16)

    put(send_small, 2 * vec_cols, jnp.dot(lhs, w_step_ref[layer], preferred_element_type=F32))
    put(send_small, 2 * vec_cols + heads, jnp.broadcast_to(squares, (squares.shape[0], 128)))
    load_vec.wait()
    for role in range(2):
        put(send_small, role * vec_cols, jnp.dot(lhs, w_vec_buf[role], preferred_element_type=F32))
    copies = deal(send_small, recv_small, sems[0], sems[1], "dp", ndp)
    block = min(cols, 512)
    for role in (0, 1):
        target, landing = ((send_gate, recv_gate), (send_val, recv_val))[role]
        load_in[role].wait()
        for at in range(0, cols, block):
            put(
                target,
                at,
                jnp.dot(lhs, w_in_buf[role, :, at : at + block], preferred_element_type=F32),
            )
        copies += deal(target, landing, sems[2 + 2 * role], sems[3 + 2 * role], "dp", ndp)
    for copy in copies:
        copy.wait()

    def total(mine, others):
        acc = mine[me].astype(F32)
        for k in range(1, ndp):
            acc = acc + others[k].astype(F32)
        return acc

    small = total(send_small, recv_small)
    own_sq = small[:, 2 * vec_cols + heads : 2 * vec_cols + heads + 1]
    scale = lax.rsqrt(own_sq * (1.0 / MODEL_WIDTH) + EPS)
    for role in range(2):
        vecs_ref[role] = (small[:, role * vec_cols : (role + 1) * vec_cols] * scale).astype(BF16)
    step_ref[...] = small[:, 2 * vec_cols : 2 * vec_cols + heads] * scale
    proj_ref[0] = (total(send_gate, recv_gate) * scale).astype(BF16)
    proj_ref[1] = (total(send_val, recv_val) * scale).astype(BF16)


def first_kernel(
    ntp, ndp, x_ref, gain_ref, w_step_ref, w_in_ref, w_vec_ref,
    proj_ref, vecs_ref, step_ref, all_ref,
    w_in_buf, w_vec_buf, lhs_buf, landed, send_gate, send_val, send_small,
    recv_gate, recv_val, recv_small, load_sem, ssem_x, rsem_x, *sems,
):
    rows_t = x_ref.shape[0]
    load_vec = pltpu.make_async_copy(w_vec_ref.at[0], w_vec_buf, load_sem.at[0])
    load_vec.start()
    load_in = []
    for role in range(2):
        copy = pltpu.make_async_copy(w_in_ref.at[0, role], w_in_buf.at[role], load_sem.at[1 + role])
        copy.start()
        load_in.append(copy)
    greet((("tp", ntp), ("dp", ndp)))
    copies = spread(x_ref, landed, ssem_x, rsem_x, "tp", ntp)
    landed[lax.axis_index("tp")] = x_ref[...]
    gain = gain_ref[...].astype(F32)[0:1]
    for copy in copies:
        copy.wait()
    squares = []
    for i in range(ntp):
        part = landed[i]
        all_ref[i] = part
        part = part.astype(F32)
        squares.append(jnp.sum(part * part, axis=1, keepdims=True))
        lhs_buf[i * rows_t : (i + 1) * rows_t, :] = part * gain
    squares = jnp.concatenate(squares, axis=0)
    project(
        0, ndp, proj_ref.shape[1], lhs_buf[...].astype(BF16), squares, (w_in_buf, w_vec_buf),
        (load_in, load_vec), w_step_ref, (send_gate, send_val, send_small),
        (recv_gate, recv_val, recv_small), sems, (proj_ref, vecs_ref, step_ref),
    )


def gather_normed(ndp, normed_ref, held, lhs_out, send_sem, recv_sem):
    rows_d = normed_ref.shape[0]
    copies = spread(normed_ref, held, send_sem, recv_sem, "dp", ndp)
    held[lax.axis_index("dp")] = normed_ref[...]
    for copy in copies:
        copy.wait()
    for i in range(ndp):
        lhs_out[i * rows_d : (i + 1) * rows_d, :] = held[i].astype(F32)
    return lhs_out[...].astype(BF16)


def middle_kernel(
    layer, ntp, ndp, normed_ref, old_ref, gain_ref, w_step_ref, w_out_ref, w_in_ref, w_vec_ref,
    proj_ref, vecs_ref, step_ref, all_ref,
    w_out_buf, w_in_buf, w_vec_buf, lhs_out, lhs_buf, held, part_out, parts_in,
    send_gate, send_val, send_small, recv_gate, recv_val, recv_small,
    load_sem, ssem_n, rsem_n, ssem_o, rsem_o, *sems,
):
    rows_t = old_ref.shape[1]
    load_out = pltpu.make_async_copy(w_out_ref.at[layer - 1], w_out_buf, load_sem.at[3])
    load_out.start()
    load_vec = pltpu.make_async_copy(w_vec_ref.at[layer], w_vec_buf, load_sem.at[0])
    load_vec.start()
    load_in = []
    for role in range(2):
        copy = pltpu.make_async_copy(
            w_in_ref.at[layer, role], w_in_buf.at[role], load_sem.at[1 + role]
        )
        copy.start()
        load_in.append(copy)
    greet((("tp", ntp), ("dp", ndp)))
    lhs = gather_normed(ndp, normed_ref, held, lhs_out, ssem_n, rsem_n)
    gain = gain_ref[...].astype(F32)[layer : layer + 1]
    load_out.wait()
    part_out[...] = jnp.dot(lhs, w_out_buf[...], preferred_element_type=F32).astype(BF16)
    copies = deal(part_out, parts_in, ssem_o, rsem_o, "tp", ntp, whole=True)
    for copy in copies:
        copy.wait()
    acc = part_out[...].astype(F32)
    for k in range(1, ntp):
        acc = acc + parts_in[k].astype(F32)
    squares = []
    for i in range(ntp):
        part = (old_ref[i].astype(F32) + acc[i * rows_t : (i + 1) * rows_t]).astype(BF16)
        all_ref[i] = part
        part = part.astype(F32)
        squares.append(jnp.sum(part * part, axis=1, keepdims=True))
        lhs_buf[i * rows_t : (i + 1) * rows_t, :] = part * gain
    squares = jnp.concatenate(squares, axis=0)
    project(
        layer, ndp, proj_ref.shape[1], lhs_buf[...].astype(BF16), squares, (w_in_buf, w_vec_buf),
        (load_in, load_vec), w_step_ref, (send_gate, send_val, send_small),
        (recv_gate, recv_val, recv_small), sems, (proj_ref, vecs_ref, step_ref),
    )


def last_kernel(
    layer, ntp, ndp, normed_ref, old_ref, w_out_ref, out_ref,
    w_out_buf, lhs_out, held, send_out, recv_out, load_sem, ssem_n, rsem_n, ssem_o, rsem_o,
):
    rows_t = old_ref.shape[1]
    load_out = pltpu.make_async_copy(w_out_ref.at[layer], w_out_buf, load_sem)
    load_out.start()
    greet((("tp", ntp), ("dp", ndp)))
    lhs = gather_normed(ndp, normed_ref, held, lhs_out, ssem_n, rsem_n)
    load_out.wait()
    acc = jnp.dot(lhs, w_out_buf[...], preferred_element_type=F32)
    for i in range(ntp):
        send_out[i] = acc[i * rows_t : (i + 1) * rows_t].astype(BF16)
    me = lax.axis_index("tp")
    copies = deal(send_out, recv_out, ssem_o, rsem_o, "tp", ntp)
    for copy in copies:
        copy.wait()
    acc = send_out[me].astype(F32)
    for k in range(1, ntp):
        acc = acc + recv_out[k].astype(F32)
    out_ref[...] = (old_ref[me].astype(F32) + acc).astype(BF16)


VMEM = pl.BlockSpec(memory_space=pltpu.VMEM)
HBM = pl.BlockSpec(memory_space=pl.ANY)


def sizes_of(tokens, w_in, w_vec, w_step, ntp, ndp):
    rows_t, width = tokens.shape
    batch = rows_t * ntp
    return rows_t, width, batch, batch // ndp, w_in.shape[3], w_vec.shape[3], w_step.shape[2]


def dma(n):
    return pltpu.SemaphoreType.DMA((n,))


def mixer_scratch(width, cols, vcols, heads, rows_d, ndp):
    small = 2 * vcols + heads + 128
    return [
        pltpu.VMEM((2, width, cols), BF16),
        pltpu.VMEM((2, width, vcols), BF16),
    ], [
        pltpu.VMEM((ndp, rows_d, cols), BF16),
        pltpu.VMEM((ndp, rows_d, cols), BF16),
        pltpu.VMEM((ndp, rows_d, small), BF16),
        pltpu.VMEM((ndp, rows_d, cols), BF16),
        pltpu.VMEM((ndp, rows_d, cols), BF16),
        pltpu.VMEM((ndp, rows_d, small), BF16),
    ]


def first_call(ntp, ndp, tokens, mix_gain, w_step, w_in, w_vec):
    rows_t, width, batch, rows_d, cols, vcols, heads = sizes_of(
        tokens, w_in, w_vec, w_step, ntp, ndp
    )
    bufs, wires = mixer_scratch(width, cols, vcols, heads, rows_d, ndp)
    return pl.pallas_call(
        functools.partial(first_kernel, ntp, ndp),
        out_shape=(
            jax.ShapeDtypeStruct((2, rows_d, cols), BF16),
            jax.ShapeDtypeStruct((2, rows_d, vcols), BF16),
            jax.ShapeDtypeStruct((rows_d, heads), F32),
            jax.ShapeDtypeStruct((ntp, rows_t, width), BF16),
        ),
        in_specs=[VMEM, VMEM, VMEM, HBM, HBM],
        out_specs=(VMEM,) * 4,
        scratch_shapes=bufs
        + [pltpu.VMEM((batch, width), F32), pltpu.VMEM((ntp, rows_t, width), BF16)]
        + wires
        + [dma(3), dma(ntp), dma(ntp)]
        + [dma(ndp)] * 6,
        compiler_params=pltpu.CompilerParams(collective_id=0, has_side_effects=True),
    )(tokens, mix_gain, w_step, w_in, w_vec)


def middle_call(layer, ntp, ndp, tokens, normed, old, mix_gain, w_step, w_out, w_in, w_vec):
    rows_t, width, batch, rows_d, cols, vcols, heads = sizes_of(
        tokens, w_in, w_vec, w_step, ntp, ndp
    )
    bufs, wires = mixer_scratch(width, cols, vcols, heads, rows_d, ndp)
    return pl.pallas_call(
        functools.partial(middle_kernel, layer, ntp, ndp),
        out_shape=(
            jax.ShapeDtypeStruct((2, rows_d, cols), BF16),
            jax.ShapeDtypeStruct((2, rows_d, vcols), BF16),
            jax.ShapeDtypeStruct((rows_d, heads), F32),
            jax.ShapeDtypeStruct((ntp, rows_t, width), BF16),
        ),
        in_specs=[VMEM, VMEM, VMEM, VMEM, HBM, HBM, HBM],
        out_specs=(VMEM,) * 4,
        scratch_shapes=[pltpu.VMEM((cols, width), BF16)]
        + bufs
        + [
            pltpu.VMEM((batch, cols), F32),
            pltpu.VMEM((batch, width), F32),
            pltpu.VMEM((ndp, rows_d, cols), BF16),
            pltpu.VMEM((batch, width), BF16),
            pltpu.VMEM((ntp, batch, width), BF16),
        ]
        + wires
        + [dma(4), dma(ndp), dma(ndp), dma(ntp), dma(ntp)]
        + [dma(ndp)] * 6,
        compiler_params=pltpu.CompilerParams(collective_id=layer, has_side_effects=True),
    )(normed, old, mix_gain, w_step, w_out, w_in, w_vec)


def last_call(layer, ntp, ndp, normed, old, w_out):
    _, rows_t, width = old.shape
    rows_d, cols = normed.shape
    batch = rows_t * ntp
    return pl.pallas_call(
        functools.partial(last_kernel, layer, ntp, ndp),
        out_shape=jax.ShapeDtypeStruct((rows_t, width), BF16),
        in_specs=[VMEM, VMEM, HBM],
        out_specs=VMEM,
        scratch_shapes=[
            pltpu.VMEM((cols, width), BF16),
            pltpu.VMEM((batch, cols), F32),
            pltpu.VMEM((ndp, rows_d, cols), BF16),
            pltpu.VMEM((ntp, rows_t, width), BF16),
            pltpu.VMEM((ntp, rows_t, width), BF16),
            pltpu.SemaphoreType.DMA,
            dma(ndp), dma(ndp), dma(ntp), dma(ntp),
        ],
        compiler_params=pltpu.CompilerParams(collective_id=layer + 1, has_side_effects=True),
    )(normed, old, w_out)


def head_step(
    layer, proj, vecs, step_all, conv_weight, conv_vec, conv_state, vec_state, ssm_state,
    step_bias, decay_log, skip_gain, out_gain,
):
    local_rows, columns = proj.shape[1:]
    vec_columns = vecs.shape[2]
    local_heads = ssm_state.shape[2]
    head_start = lax.axis_index("tp") * local_heads
    step_raw = lax.dynamic_slice_in_dim(step_all, head_start, local_heads, 1)
    window = jnp.concatenate([conv_state[layer], proj[1][:, None, :]], axis=1)
    new_conv = window[:, 1:, :]
    values_sum = jnp.sum(
        window.astype(jnp.float32) * conv_weight[layer].astype(jnp.float32)[None, :, :], axis=1
    )
    fresh = vecs[:, :, None, :]
    vec_window = jnp.concatenate([vec_state[layer], fresh], axis=2)
    new_vec = vec_window[:, :, 1:, :]
    vec_sum = jnp.sum(
        vec_window.astype(jnp.float32) * conv_vec[layer].astype(jnp.float32)[:, None, :, :], axis=2
    )
    values = jax.nn.silu(values_sum).reshape(local_rows, local_heads, HEAD_DIM)
    vec_act = jax.nn.silu(vec_sum)
    local_groups = vec_columns // STATE_DIM
    repeat = HEAD_COUNT // GROUP_COUNT
    in_vec = jnp.repeat(vec_act[0].reshape(local_rows, local_groups, STATE_DIM), repeat, axis=1)
    out_vec = jnp.repeat(vec_act[1].reshape(local_rows, local_groups, STATE_DIM), repeat, axis=1)
    step = jax.nn.softplus(step_raw + step_bias[layer][None, :])
    decay = jnp.exp(-step * jnp.exp(decay_log[layer])[None, :])
    state = (
        decay[:, :, None, None] * ssm_state[layer]
        + (step[:, :, None] * values)[..., None] * in_vec[:, :, None, :]
    )
    read = jnp.einsum("bhpn,bhn->bhp", state, out_vec) + skip_gain[layer][None, :, None] * values
    mixed = read.reshape(local_rows, columns) * jax.nn.silu(proj[0].astype(jnp.float32))
    grouped = mixed.reshape(local_rows, local_groups, columns // local_groups)
    grouped = grouped * lax.rsqrt(jnp.mean(grouped * grouped, axis=2, keepdims=True) + EPS)
    normed = (grouped.reshape(local_rows, columns) * out_gain[layer].astype(jnp.float32)).astype(
        jnp.bfloat16
    )
    return (normed, new_conv, new_vec, (decay, step[:, :, None] * values, in_vec))


def shards(
    ntp,
    ndp,
    tokens,
    w_in,
    w_vec,
    w_step,
    conv_weight,
    conv_vec,
    conv_state,
    vec_state,
    ssm_state,
    step_bias,
    decay_log,
    skip_gain,
    mix_gain,
    out_gain,
    w_out,
):
    convs = []
    vec_rows = []
    states = []
    for layer in range(LAYER_COUNT):
        if layer == 0:
            proj, vecs, step_all, rows = first_call(
                ntp, ndp, tokens, mix_gain, w_step, w_in, w_vec
            )
        else:
            proj, vecs, step_all, rows = middle_call(
                layer, ntp, ndp, tokens, normed, rows, mix_gain, w_step, w_out, w_in, w_vec
            )
        normed, conv_next, vec_next, state_next = head_step(
            layer, proj, vecs, step_all, conv_weight, conv_vec, conv_state, vec_state,
            ssm_state, step_bias, decay_log, skip_gain, out_gain,
        )
        convs.append(conv_next)
        vec_rows.append(vec_next)
        states.append(state_next)
    current = last_call(LAYER_COUNT - 1, ntp, ndp, normed, rows, w_out)
    decays, drives, inputs = (jnp.stack(parts) for parts in zip(*states))
    new_ssm = (
        decays[..., None, None] * ssm_state + drives[..., None] * inputs[:, :, :, None, :]
    )
    return (current, jnp.stack(convs), jnp.stack(vec_rows), new_ssm)


def solution(mesh):
    placed = (
        P(("grp", "tp"), "dp"),
        P(None, None, "dp", "tp"),
        P(None, None, "dp", "tp"),
        P(None, "dp", None),
        P(None, None, "tp"),
        P(None, None, None, "tp"),
        P(None, ("grp", "dp"), None, "tp"),
        P(None, None, ("grp", "dp"), None, "tp"),
        P(None, ("grp", "dp"), "tp", None, None),
        P(None, "tp"),
        P(None, "tp"),
        P(None, "tp"),
        P(None, "dp"),
        P(None, "tp"),
        P(None, "tp", "dp"),
    )
    return jax.shard_map(
        functools.partial(shards, mesh.shape["tp"], mesh.shape["dp"]),
        mesh=mesh,
        in_specs=placed,
        out_specs=(
            P(("grp", "tp"), "dp"),
            P(None, ("grp", "dp"), None, "tp"),
            P(None, None, ("grp", "dp"), None, "tp"),
            P(None, ("grp", "dp"), "tp", None, None),
        ),
        check_vma=False,
    )
```
